32 devices in a mesh: tp: 8 (over z, core), dp: 4 (over y, x).
Axes of the slice: x: 2, y: 2, z: 4, core: 2. Of those that a mesh axis runs over, the one named last changes fastest.
Arguments:
- tokens: bfloat16 [128, 2048], P(None, 'dp'), may hold values from -21 to 21
- lengths: int32 [8], P('dp'), may hold values from 1 to 16, 42 in all
- input_norm_scale: float32 [2, 2048], P(None, 'dp'), may hold values from 0.1 to 1.9
- gate_input_weight: bfloat16 [2, 2048, 2, 2048], P(None, 'dp', None, 'tp'), may hold values from -0.125 to 0.125
- maps_weight: bfloat16 [2, 2048, 2, 512], P(None, 'dp', None, 'tp'), may hold values from -0.125 to 0.125
- step_weight: bfloat16 [2, 2048, 32], P(None, 'dp', 'tp'), may hold values from -0.125 to 0.125
- input_tap_weight: bfloat16 [2, 4, 2048], P(None, None, 'tp'), may hold values from -3 to 3
- map_tap_weight: bfloat16 [2, 4, 2, 512], P(None, None, None, 'tp'), may hold values from -3 to 3
- step_size_bias: float32 [2, 32], P(None, 'tp'), may hold values from -4 to -1
- decay_rate_logarithm: float32 [2, 32], P(None, 'tp'), may hold values from -2 to 2.5
- direct_path_weight: float32 [2, 32], P(None, 'tp'), may hold values from 0.25 to 2.5
- head_norm_scale: float32 [2, 2048], P(None, 'tp'), may hold values from 0.1 to 1.9
- output_weight: bfloat16 [2, 2048, 2048], P(None, 'tp', 'dp'), may hold values from -0.125 to 0.125
- convolution_input_cache: bfloat16 [2, 8, 3, 2048], P(None, 'dp', None, 'tp'), may hold values from -6 to 6
- convolution_map_cache: bfloat16 [2, 8, 3, 2, 512], P(None, 'dp', None, None, 'tp'), may hold values from -6 to 6
- recurrent_state: float32 [2, 8, 32, 64, 128], P(None, 'dp', 'tp'), may hold values from -6 to 6
- extra_log_decay: float32 [2, 8, 16, 32], P(None, 'dp', None, 'tp'), may hold values from -0.7 to 0, as said below
Outputs:
- stream_out: float32 [128, 2048], P(None, 'dp')
- conv_input_out: bfloat16 [2, 8, 3, 2048], P(None, 'dp', None, 'tp')
- conv_maps_out: bfloat16 [2, 8, 3, 2, 512], P(None, 'dp', None, None, 'tp')
- ssm_out: float32 [2, 8, 32, 64, 128], P(None, 'dp', 'tp')
The draws below stay inside these ranges and needn't reach their ends.
Inputs may be any that keep to these rules, and one draw needn't show every extreme that they name: `extra_log_decay`: zero at most slots, a drop of a fifth to a half of the state at a few.
All inputs are finite; a program needn't handle non-finite values. No bound on the sum of `lengths` on one device may be relied on, other than what follows from the above.
Results may differ from the reference program's by a relative error of at most 0.04.
Values may be sent and summed in bfloat16 or wider, within the bound.
No kernel may reach another device: no remote copies, remote signals or barrier semaphores. Data moves between devices by JAX's collectives and lax.ppermute only.
A program may use at most 64 MiB of HBM per device.

```python
import math
import jax
import jax.numpy as jnp
import numpy as np
from jax import lax

D = 2048
STATE_HEADS = 32
P_SIZE = 64
N = 128
G = 4
CONV = 4
TOKEN_SLOTS = 16
MIXER_LAYERS = 2
INNER = 2048
GN = 512
SEQUENCE_COUNT = 8
TOKENS = 128
DP_ROWS = 512
N_DP = 4


def draw_tokens(key, part):
    random_key_first, random_key_second = jax.random.split(key, 2)
    base_draw = jnp.clip(jax.random.normal(random_key_first, (TOKENS, D), jnp.float32), -4.0, 4.0)
    column = jnp.exp(jnp.linspace(math.log(0.5), math.log(3.0), D)) * jax.random.uniform(random_key_second, (D,), jnp.float32, 0.7, 1.0)
    return (base_draw * column[None, :]).astype(jnp.bfloat16)


def draw_extra_log_decay(key, part):
    random_key_first, random_key_second = jax.random.split(key)
    spike_hits = jax.random.randint(random_key_first, (MIXER_LAYERS, SEQUENCE_COUNT, TOKEN_SLOTS, STATE_HEADS), 0, 12) == 0
    spike_depth = jax.random.uniform(random_key_second, (MIXER_LAYERS, SEQUENCE_COUNT, TOKEN_SLOTS, STATE_HEADS), jnp.float32, math.log(0.5), math.log(0.8))
    return jnp.where(spike_hits, spike_depth, 0.0).astype(jnp.float32)


def level_of(own_key, dims, cuts, smallest, largest):
    level, own = 1.0, jax.random.fold_in(own_key, 6)
    for axis_at, shards_of in cuts:
        steps = jnp.exp(jax.random.uniform(jax.random.fold_in(own, axis_at), (shards_of,), jnp.float32, smallest / len(cuts), largest / len(cuts)))
        level = level * jnp.repeat(steps, dims[axis_at] // shards_of).reshape([-1 if axis == axis_at else 1 for axis in range(len(dims))])
    return level


def split_up(number_of, total, reach, slope):
    loads = [(1 << 20) // math.isqrt(grade ** slope) + 1 for grade in range(2, number_of + 1)]
    surplus, holding = total - reach - (number_of - 1), [1] * (number_of - 1)
    while surplus > 0:
        candidates = [i for i in range(number_of - 1) if holding[i] < reach]
        mass, remaining = sum([loads[i] for i in candidates]), surplus
        for i in candidates:
            more = min(reach - holding[i], max(1, remaining * loads[i] // mass), surplus)
            holding[i] = holding[i] + more
            surplus = surplus - more
    return np.array([reach] + holding)


def ragged(stream_key, number_of, total, most, skew):
    if number_of == 2:
        one = jax.random.randint(stream_key, (), max(1, total - most), min(most, total - 1) + 1)
        return jnp.stack([one, total - one])
    sizes = jnp.asarray(split_up(number_of, total, most, skew), jnp.int32)
    twos = (number_of - 1) // 2
    source_of, taker = sizes[1:1 + 2 * twos:2], sizes[2:2 + 2 * twos:2]
    room = jnp.minimum(source_of - 1, most - taker)
    shifted = jax.random.randint(jax.random.fold_in(stream_key, 1), (twos,), 0, 1 << 20) % (room + 1)
    sizes = sizes.at[1:1 + 2 * twos:2].set(source_of - shifted).at[2:2 + 2 * twos:2].set(taker + shifted)
    return sizes[jax.random.permutation(jax.random.fold_in(stream_key, 2), number_of)]


def scatter_about(own_key, dims, spread, bound, pieces=(), held_as=jnp.bfloat16):
    gain = level_of(own_key, dims, pieces, -0.22, 0.18) if pieces else 1.0
    entries = jax.random.normal(own_key, dims, jnp.float32) * spread * gain
    return jnp.minimum(jnp.maximum(entries, -bound), bound).astype(held_as)


def setup_inputs(seed: int = 0) -> dict:
    arg_keys = jax.random.split(jax.random.key(seed), 18)
    return {
        "tokens": draw_tokens(jax.random.fold_in(arg_keys[17], 71), 0),
        "lengths": ragged(arg_keys[1], SEQUENCE_COUNT, SEQUENCE_COUNT * TOKEN_SLOTS // 3, TOKEN_SLOTS, 2).astype(jnp.int32),
        "input_norm_scale": jnp.clip(1.0 + 0.18 * jax.random.normal(arg_keys[2], (MIXER_LAYERS, D), jnp.float32), 0.1, 1.9),
        "gate_input_weight": scatter_about(arg_keys[3], (MIXER_LAYERS, D, 2, INNER), D ** -0.5, 0.125, ((1, 4), (3, 8))),
        "maps_weight": scatter_about(arg_keys[4], (MIXER_LAYERS, D, 2, GN), D ** -0.5, 0.125, ((1, 4), (3, 8))),
        "step_weight": scatter_about(arg_keys[5], (MIXER_LAYERS, D, STATE_HEADS), D ** -0.5, 0.125, ((1, 4), (2, 8))),
        "input_tap_weight": scatter_about(arg_keys[6], (MIXER_LAYERS, CONV, INNER), CONV ** -0.5, 3.0, ((2, 8),)),
        "map_tap_weight": scatter_about(arg_keys[7], (MIXER_LAYERS, CONV, 2, GN), CONV ** -0.5, 3.0, ((3, 8),)),
        "step_size_bias": jnp.clip(-4.0 + 3.0 * jax.random.uniform(arg_keys[8], (MIXER_LAYERS, STATE_HEADS), jnp.float32) ** level_of(arg_keys[8], (MIXER_LAYERS, STATE_HEADS), ((1, 8),), -0.2, 0.2), -4.0, -1.0),
        "decay_rate_logarithm": jnp.clip(-2.0 + 4.5 * jax.random.uniform(arg_keys[9], (MIXER_LAYERS, STATE_HEADS), jnp.float32) ** level_of(arg_keys[9], (MIXER_LAYERS, STATE_HEADS), ((1, 8),), -0.2, 0.2), -2.0, 2.5),
        "direct_path_weight": jnp.clip(jnp.exp(math.log(2.5) - 2.3025851 * jax.random.uniform(arg_keys[10], (MIXER_LAYERS, STATE_HEADS), jnp.float32) ** level_of(arg_keys[10], (MIXER_LAYERS, STATE_HEADS), ((1, 8),), -0.2, 0.2)), 0.25, 2.5),
        "head_norm_scale": jnp.clip(1.0 + 0.18 * jax.random.normal(arg_keys[11], (MIXER_LAYERS, INNER), jnp.float32), 0.1, 1.9),
        "output_weight": scatter_about(arg_keys[12], (MIXER_LAYERS, INNER, D), INNER ** -0.5, 0.125, ((1, 8), (2, 4))),
        "convolution_input_cache": scatter_about(arg_keys[13], (MIXER_LAYERS, SEQUENCE_COUNT, 3, INNER), 1.0, 6.0, ((1, 4), (3, 8))),
        "convolution_map_cache": scatter_about(arg_keys[14], (MIXER_LAYERS, SEQUENCE_COUNT, 3, 2, GN), 1.0, 6.0, ((1, 4), (4, 8))),
        "recurrent_state": scatter_about(arg_keys[15], (MIXER_LAYERS, SEQUENCE_COUNT, STATE_HEADS, P_SIZE, N), 1.0, 6.0, ((1, 4), (2, 8)), jnp.float32),
        "extra_log_decay": draw_extra_log_decay(jax.random.fold_in(arg_keys[17], 71), 0),
    }


epsilon = 1e-06
highest = lax.Precision.HIGHEST

def conv_step(previous, incoming, weights, lengths):
    padded = jnp.concatenate([previous, incoming], axis=1).astype(jnp.float32)
    taps = weights.shape[0]
    fresh_tokens = incoming.shape[1]
    filtered = padded[:, :fresh_tokens] * weights[0].astype(jnp.float32)
    for tap_index in range(1, taps):
        filtered = filtered + padded[:, tap_index:tap_index + fresh_tokens] * weights[tap_index].astype(jnp.float32)
    position = jnp.arange(fresh_tokens + taps - 1, dtype=jnp.int32)
    wanted = lengths[:, None] + jnp.arange(taps - 1, dtype=jnp.int32)[None, :]
    chooser = (position[None, None, :] == wanted[:, :, None]).astype(jnp.float32)
    kept_rows = jnp.einsum('skp,sp...->sk...', chooser, padded, precision=highest)
    return (jax.nn.silu(filtered), kept_rows.astype(jnp.bfloat16))

def ssd_block(head_input, head_gate, head_step_size, decay_logarithm, write_map, read_map, state_old, skip, gain_heads):
    decay_sum = jnp.cumsum(decay_logarithm, axis=1)
    slots = decay_logarithm.shape[1]
    causal = jnp.arange(slots)[:, None] >= jnp.arange(slots)[None, :]
    decay_gap = decay_sum[:, :, None, :] - decay_sum[:, None, :, :]
    segment = jnp.exp(jnp.where(causal[None, :, :, None], decay_gap, -jnp.inf))
    intersection = jnp.einsum('slhn,smhn->slmh', read_map, write_map, precision=highest)
    within = jnp.einsum('slmh,smh,smhp->slhp', intersection * segment, head_step_size, head_input, precision=highest)
    carried = jnp.einsum('slhn,shpn->slhp', read_map, state_old, precision=highest) * jnp.exp(decay_sum)[..., None]
    to_end = jnp.exp(decay_sum[:, -1:, :] - decay_sum)
    state_new = jnp.exp(decay_sum[:, -1])[..., None, None] * state_old + jnp.einsum('smhn,smh,smhp->shpn', write_map, to_end * head_step_size, head_input, precision=highest)
    mixed_out = within + carried + skip[:, None] * head_input
    mixed_out = mixed_out * jax.nn.silu(head_gate)
    mixed_out = mixed_out * lax.rsqrt(lax.optimization_barrier(jnp.mean(mixed_out * mixed_out, axis=-1, keepdims=True)) + epsilon) * gain_heads
    return (mixed_out, state_new)

def reference(tokens, lengths, input_norm_scale, gate_input_weight, maps_weight, step_weight, input_tap_weight, map_tap_weight, step_size_bias, decay_rate_logarithm, direct_path_weight, head_norm_scale, output_weight, convolution_input_cache, convolution_map_cache, recurrent_state, extra_log_decay):
    stream = tokens.astype(jnp.float32)
    active_mask = (jnp.arange(TOKEN_SLOTS, dtype=jnp.int32)[None, :] < lengths[:, None]).astype(jnp.float32)
    input_states, map_states, ssm_states = ([], [], [])
    per_group = STATE_HEADS // G
    for layer_number in range(MIXER_LAYERS):
        stream_f = stream
        factor = lax.rsqrt(lax.optimization_barrier(jnp.sum(stream_f * stream_f, axis=1, keepdims=True)) / D + epsilon)
        normed = (stream_f * input_norm_scale[layer_number]).astype(jnp.bfloat16)
        weight_all = jnp.concatenate([gate_input_weight[layer_number].reshape(D, 2 * INNER), maps_weight[layer_number].reshape(D, 2 * GN), step_weight[layer_number]], axis=1)
        total_cols = weight_all.shape[1]
        row_pieces = normed.reshape(TOKENS, N_DP, DP_ROWS).transpose(1, 0, 2)
        weight_pieces = weight_all.reshape(N_DP, DP_ROWS, total_cols)

        def add_block(running, pair_item):
            partial_prod = jnp.dot(pair_item[0], pair_item[1], preferred_element_type=jnp.float32)
            rounded = lax.optimization_barrier(partial_prod.astype(jnp.bfloat16))
            return (running + rounded.astype(jnp.float32), None)
        proj_sum, _ = lax.scan(add_block, jnp.zeros((TOKENS, total_cols), jnp.float32), (row_pieces, weight_pieces))
        projected = (proj_sum * factor).astype(jnp.bfloat16)
        gate_input = projected[:, :2 * INNER].reshape(SEQUENCE_COUNT, TOKEN_SLOTS, 2, INNER)
        map_input = projected[:, 2 * INNER:2 * INNER + 2 * GN].reshape(SEQUENCE_COUNT, TOKEN_SLOTS, 2, GN)
        step_raw = projected[:, 2 * INNER + 2 * GN:].reshape(SEQUENCE_COUNT, TOKEN_SLOTS, STATE_HEADS)
        conv_input, input_kept = conv_step(convolution_input_cache[layer_number], gate_input[:, :, 1], input_tap_weight[layer_number], lengths)
        maps_f, maps_kept = conv_step(convolution_map_cache[layer_number], map_input, map_tap_weight[layer_number], lengths)
        maps = maps_f.astype(jnp.bfloat16)
        write_groups = maps[:, :, 0].reshape(SEQUENCE_COUNT, TOKEN_SLOTS, N, G).transpose(0, 1, 3, 2)
        read_groups = maps[:, :, 1].reshape(SEQUENCE_COUNT, TOKEN_SLOTS, N, G).transpose(0, 1, 3, 2)
        write_map = jnp.repeat(write_groups, per_group, axis=2).astype(jnp.float32)
        read_map = jnp.repeat(read_groups, per_group, axis=2).astype(jnp.float32)
        head_step_size = jax.nn.softplus(step_raw.astype(jnp.float32) + step_size_bias[layer_number]) * active_mask[..., None]
        decay_logarithm = head_step_size * -jnp.exp(decay_rate_logarithm[layer_number]) + extra_log_decay[layer_number] * active_mask[..., None]
        head_input = conv_input.reshape(SEQUENCE_COUNT, TOKEN_SLOTS, STATE_HEADS, P_SIZE)
        head_gate = gate_input[:, :, 0].astype(jnp.float32).reshape(SEQUENCE_COUNT, TOKEN_SLOTS, STATE_HEADS, P_SIZE)
        mixed_out, state_new = ssd_block(head_input, head_gate, head_step_size, decay_logarithm, write_map, read_map, recurrent_state[layer_number], direct_path_weight[layer_number], head_norm_scale[layer_number].reshape(STATE_HEADS, P_SIZE))
        head_out = (mixed_out * active_mask[:, :, None, None]).astype(jnp.bfloat16).reshape(TOKENS, INNER)
        projected_out = jnp.dot(head_out, output_weight[layer_number], preferred_element_type=jnp.float32)
        stream = stream_f + projected_out
        input_states.append(input_kept)
        map_states.append(maps_kept)
        ssm_states.append(state_new)
    return (stream, jnp.stack(input_states), jnp.stack(map_states), jnp.stack(ssm_states))
```

```python
import jax
import jax.numpy as jnp
from jax import lax
from jax.sharding import PartitionSpec as P

D = 2048
STATE_HEADS = 32
N = 128
G = 4
MIXER_LAYERS = 2


epsilon = 1e-06
highest = lax.Precision.HIGHEST


def conv_step(previous, incoming, weights, lengths):
    padded = jnp.concatenate([previous, incoming], axis=1).astype(jnp.float32)
    taps = weights.shape[0]
    fresh_tokens = incoming.shape[1]
    filtered = padded[:, :fresh_tokens] * weights[0].astype(jnp.float32)
    for tap_index in range(1, taps):
        filtered = filtered + padded[:, tap_index : tap_index + fresh_tokens] * weights[
            tap_index
        ].astype(jnp.float32)
    position = jnp.arange(fresh_tokens + taps - 1, dtype=jnp.int32)
    wanted = lengths[:, None] + jnp.arange(taps - 1, dtype=jnp.int32)[None, :]
    chooser = (position[None, None, :] == wanted[:, :, None]).astype(jnp.float32)
    kept_rows = jnp.einsum("skp,sp...->sk...", chooser, padded, precision=highest)
    return (jax.nn.silu(filtered), kept_rows.astype(jnp.bfloat16))


def ssd_block(
    head_input,
    head_gate,
    head_step_size,
    decay_logarithm,
    write_map,
    read_map,
    state_old,
    skip,
    gain_heads,
):
    decay_sum = jnp.cumsum(decay_logarithm, axis=1)
    slots = decay_logarithm.shape[1]
    causal = jnp.arange(slots)[:, None] >= jnp.arange(slots)[None, :]
    decay_gap = decay_sum[:, :, None, :] - decay_sum[:, None, :, :]
    segment = jnp.exp(jnp.where(causal[None, :, :, None], decay_gap, -jnp.inf))
    intersection = jnp.einsum("sln,smn->slm", read_map, write_map, precision=highest)[..., None]
    within = jnp.einsum(
        "slmh,smh,smhp->slhp", intersection * segment, head_step_size, head_input, precision=highest
    )
    carried = (
        jnp.einsum("sln,shpn->slhp", read_map, state_old, precision=highest)
        * jnp.exp(decay_sum)[..., None]
    )
    to_end = jnp.exp(decay_sum[:, -1:, :] - decay_sum)
    state_new = jnp.exp(decay_sum[:, -1])[..., None, None] * state_old + jnp.einsum(
        "smn,smh,smhp->shpn", write_map, to_end * head_step_size, head_input, precision=highest
    )
    mixed_out = within + carried + skip[:, None] * head_input
    mixed_out = mixed_out * jax.nn.silu(head_gate)
    mixed_out = (
        mixed_out
        * lax.rsqrt(jnp.mean(mixed_out * mixed_out, axis=-1, keepdims=True) + epsilon)
        * gain_heads
    )
    return (mixed_out, state_new)


def partner(rank, step, count):
    return rank ^ step if count & (count - 1) == 0 else (rank + step) % count


def send_to(block, axis, step, count, stride=1):
    width = count * stride
    pairs = [(r, partner(r // stride, step, count) * stride + r % stride) for r in range(width)]
    return lax.ppermute(block, axis, pairs)


def take_from(block, axis, step, count, stride=1):
    width = count * stride
    pairs = [(partner(r // stride, step, count) * stride + r % stride, r) for r in range(width)]
    return lax.ppermute(block, axis, pairs)


def body(
    tokens,
    lengths,
    input_norm_scale,
    gate_input_weight,
    maps_weight,
    step_weight,
    input_tap_weight,
    map_tap_weight,
    step_size_bias,
    decay_rate_logarithm,
    direct_path_weight,
    head_norm_scale,
    output_weight,
    convolution_input_cache,
    convolution_map_cache,
    recurrent_state,
    extra_log_decay,
):
    head_rank = lax.axis_index("tp")
    seq_rank = lax.axis_index("dp")
    local_sequences = extra_log_decay.shape[1]
    fresh_tokens = extra_log_decay.shape[2]
    heads_here = step_size_bias.shape[1]
    head_size = head_norm_scale.shape[1] // heads_here
    own_rows = local_sequences * fresh_tokens
    active_mask = (jnp.arange(fresh_tokens, dtype=jnp.int32)[None, :] < lengths[:, None]).astype(
        jnp.float32
    )
    group_index = head_rank * heads_here // (STATE_HEADS // G)
    dp_count = lax.axis_size("dp")
    tp_count = lax.axis_size("tp")
    inner = 2 if tp_count % 2 == 0 else 1
    outer = tp_count // inner
    blocks = [partner(seq_rank, k, dp_count) if k else seq_rank for k in range(dp_count)]
    stream = jnp.concatenate(
        [lax.dynamic_slice_in_dim(tokens, blk * own_rows, own_rows, 0) for blk in blocks], axis=0
    ).astype(jnp.float32)
    gathered_weight = [
        [output_weight[n]]
        + [take_from(output_weight[n], "tp", k, outer, inner) for k in range(1, outer)]
        for n in range(MIXER_LAYERS)
    ]
    map_cols = maps_weight.shape[3]
    row = jnp.arange(2 * map_cols, dtype=jnp.int32)[:, None]
    col = jnp.arange(2 * N, dtype=jnp.int32)[None, :]
    selectors = []
    for k in range(tp_count):
        source = partner(head_rank, k, tp_count) if k else head_rank
        hit = (row // map_cols == col // N) & (
            source * map_cols + row % map_cols == G * (col % N) + group_index
        )
        selectors.append(hit.astype(jnp.bfloat16))
    selector = jnp.concatenate(selectors, axis=0)
    input_states, map_states, ssm_states = ([], [], [])
    for layer_number in range(MIXER_LAYERS):
        row_squares = jnp.sum(stream * stream, axis=1)
        squares_high = lax.reduce_precision(row_squares, 8, 7)
        squares_low = row_squares - squares_high
        normed = (stream * input_norm_scale[layer_number]).astype(jnp.bfloat16)
        total_rows = normed.shape[0]
        pair_partial = jnp.einsum(
            "td,dkc->tkc",
            normed,
            gate_input_weight[layer_number],
            preferred_element_type=jnp.float32,
        ).reshape(total_rows, -1)
        maps_partial = jnp.einsum(
            "td,dkc->tkc", normed, maps_weight[layer_number], preferred_element_type=jnp.float32
        ).reshape(total_rows, -1)
        step_partial = jnp.dot(
            normed, step_weight[layer_number], preferred_element_type=jnp.float32
        )
        packed = jnp.concatenate(
            [
                pair_partial.astype(jnp.bfloat16),
                maps_partial.astype(jnp.bfloat16),
                step_partial.astype(jnp.bfloat16),
                squares_high[:, None].astype(jnp.bfloat16),
                squares_low[:, None].astype(jnp.bfloat16),
            ],
            axis=1,
        )
        pieces = [packed[k * own_rows : (k + 1) * own_rows] for k in range(dp_count)]
        total = pieces[0].astype(jnp.float32)
        for k in range(1, dp_count):
            total = total + send_to(pieces[k], "dp", k, dp_count).astype(jnp.float32)
        own_factor = lax.rsqrt((total[:, -2:-1] + total[:, -1:]) / D + epsilon)
        wide = pair_partial.shape[1]
        projected = (total[:, :-2] * own_factor).astype(jnp.bfloat16)
        gate_input = projected[:, :wide].reshape(local_sequences, fresh_tokens, 2, wide // 2)
        map_input = projected[:, wide : wide + 2 * map_cols].reshape(
            local_sequences, fresh_tokens, 2, map_cols
        )
        step_raw = projected[:, wide + 2 * map_cols :].reshape(
            local_sequences, fresh_tokens, heads_here
        )
        maps_f, maps_kept = conv_step(
            convolution_map_cache[layer_number], map_input, map_tap_weight[layer_number], lengths
        )
        maps_own = maps_f.astype(jnp.bfloat16).reshape(own_rows, 2 * map_cols)
        maps_all = jnp.concatenate(
            [maps_own] + [take_from(maps_own, "tp", k, tp_count) for k in range(1, tp_count)],
            axis=1,
        )
        conv_input, input_kept = conv_step(
            convolution_input_cache[layer_number],
            gate_input[:, :, 1],
            input_tap_weight[layer_number],
            lengths,
        )
        group_maps = jnp.dot(maps_all, selector, preferred_element_type=jnp.float32).reshape(
            local_sequences, fresh_tokens, 2, N
        )
        write_map = group_maps[:, :, 0]
        read_map = group_maps[:, :, 1]
        head_step_size = (
            jax.nn.softplus(step_raw.astype(jnp.float32) + step_size_bias[layer_number])
            * active_mask[..., None]
        )
        decay_logarithm = (
            head_step_size * -jnp.exp(decay_rate_logarithm[layer_number])
            + extra_log_decay[layer_number] * active_mask[..., None]
        )
        head_input = conv_input.reshape(local_sequences, fresh_tokens, heads_here, head_size)
        head_gate = (
            gate_input[:, :, 0]
            .astype(jnp.float32)
            .reshape(local_sequences, fresh_tokens, heads_here, head_size)
        )
        mixed_out, state_new = ssd_block(
            head_input,
            head_gate,
            head_step_size,
            decay_logarithm,
            write_map,
            read_map,
            recurrent_state[layer_number],
            direct_path_weight[layer_number],
            head_norm_scale[layer_number].reshape(heads_here, head_size),
        )
        head_out = (
            (mixed_out * active_mask[:, :, None, None])
            .astype(jnp.bfloat16)
            .reshape(own_rows, heads_here * head_size)
        )
        all_rows = jnp.concatenate(
            [head_out] + [take_from(head_out, "dp", k, dp_count) for k in range(1, dp_count)],
            axis=0,
        )
        all_heads = [all_rows] + [
            take_from(all_rows, "tp", k, outer, inner) for k in range(1, outer)
        ]
        out_block = jnp.dot(
            jnp.concatenate(all_heads, axis=1),
            jnp.concatenate(gathered_weight[layer_number], axis=0),
            preferred_element_type=jnp.float32,
        )
        if inner == 2:
            pairs = [(r, r ^ 1) for r in range(tp_count)]
            out_block = out_block + lax.ppermute(out_block, "tp", pairs)
        stream = stream + out_block
        input_states.append(input_kept)
        map_states.append(maps_kept)
        ssm_states.append(state_new)
    ordered = jnp.zeros_like(stream)
    for k in range(dp_count):
        ordered = lax.dynamic_update_slice_in_dim(
            ordered, stream[k * own_rows : (k + 1) * own_rows], blocks[k] * own_rows, 0
        )
    return (ordered, jnp.stack(input_states), jnp.stack(map_states), jnp.stack(ssm_states))


def solution(mesh):
    placed = (
        P(None, "dp"),
        P("dp"),
        P(None, "dp"),
        P(None, "dp", None, "tp"),
        P(None, "dp", None, "tp"),
        P(None, "dp", "tp"),
        P(None, None, "tp"),
        P(None, None, None, "tp"),
        P(None, "tp"),
        P(None, "tp"),
        P(None, "tp"),
        P(None, "tp"),
        P(None, "tp", "dp"),
        P(None, "dp", None, "tp"),
        P(None, "dp", None, None, "tp"),
        P(None, "dp", "tp", None, None),
        P(None, "dp", None, "tp"),
    )
    return jax.shard_map(
        body,
        mesh=mesh,
        in_specs=placed,
        out_specs=(
            P(None, "dp"),
            P(None, "dp", None, "tp"),
            P(None, "dp", None, None, "tp"),
            P(None, "dp", "tp", None, None),
        ),
        check_vma=False,
    )
```

```python
import jax
import jax.numpy as jnp
from jax import lax
from jax.experimental.layout import Layout, with_layout_constraint
from jax.sharding import PartitionSpec as P

D = 2048
STATE_HEADS = 32
N = 128
G = 4
MIXER_LAYERS = 2


epsilon = 1e-06
highest = lax.Precision.HIGHEST


def conv_step(previous, incoming, weights, lengths):
    padded = jnp.concatenate([previous, incoming], axis=1).astype(jnp.float32)
    taps = weights.shape[0]
    fresh_tokens = incoming.shape[1]
    filtered = padded[:, :fresh_tokens] * weights[0].astype(jnp.float32)
    for tap_index in range(1, taps):
        filtered = filtered + padded[:, tap_index : tap_index + fresh_tokens] * weights[
            tap_index
        ].astype(jnp.float32)
    position = jnp.arange(fresh_tokens + taps - 1, dtype=jnp.int32)
    wanted = lengths[:, None] + jnp.arange(taps - 1, dtype=jnp.int32)[None, :]
    chooser = (position[None, None, :] == wanted[:, :, None]).astype(jnp.float32)
    kept_rows = jnp.einsum("skp,sp...->sk...", chooser, padded, precision=highest)
    return (jax.nn.silu(filtered), kept_rows.astype(jnp.bfloat16))


def ssd_block(
    head_input,
    head_gate,
    head_step_size,
    decay_logarithm,
    write_map,
    read_map,
    state_old,
    skip,
    gain_heads,
):
    decay_sum = jnp.cumsum(decay_logarithm, axis=1)
    slots = decay_logarithm.shape[1]
    causal = jnp.arange(slots)[:, None] >= jnp.arange(slots)[None, :]
    decay_gap = decay_sum[:, :, None, :] - decay_sum[:, None, :, :]
    segment = jnp.exp(jnp.where(causal[None, :, :, None], decay_gap, -jnp.inf))
    intersection = jnp.einsum("sln,smn->slm", read_map, write_map, precision=highest)[..., None]
    within = jnp.einsum(
        "slmh,smh,smhp->slhp", intersection * segment, head_step_size, head_input, precision=highest
    )
    carried = (
        jnp.einsum("sln,shpn->slhp", read_map, state_old, precision=highest)
        * jnp.exp(decay_sum)[..., None]
    )
    to_end = jnp.exp(decay_sum[:, -1:, :] - decay_sum)
    state_new = jnp.exp(decay_sum[:, -1])[..., None, None] * state_old + jnp.einsum(
        "smn,smh,smhp->shpn", write_map, to_end * head_step_size, head_input, precision=highest
    )
    mixed_out = within + carried + skip[:, None] * head_input
    mixed_out = mixed_out * jax.nn.silu(head_gate)
    mixed_out = (
        mixed_out
        * lax.rsqrt(jnp.mean(mixed_out * mixed_out, axis=-1, keepdims=True) + epsilon)
        * gain_heads
    )
    return (mixed_out, state_new)


def partner(rank, step, count):
    return rank ^ step if count & (count - 1) == 0 else (rank + step) % count


def send_to(block, axis, step, count, stride=1):
    width = count * stride
    pairs = [(r, partner(r // stride, step, count) * stride + r % stride) for r in range(width)]
    return lax.ppermute(block, axis, pairs)


def take_from(block, axis, step, count, stride=1):
    width = count * stride
    pairs = [(partner(r // stride, step, count) * stride + r % stride, r) for r in range(width)]
    return lax.ppermute(block, axis, pairs)


def body(
    tokens,
    lengths,
    input_norm_scale,
    gate_input_weight,
    maps_weight,
    step_weight,
    input_tap_weight,
    map_tap_weight,
    step_size_bias,
    decay_rate_logarithm,
    direct_path_weight,
    head_norm_scale,
    output_weight,
    convolution_input_cache,
    convolution_map_cache,
    recurrent_state,
    extra_log_decay,
):
    head_rank = lax.axis_index("tp")
    seq_rank = lax.axis_index("dp")
    local_sequences = extra_log_decay.shape[1]
    fresh_tokens = extra_log_decay.shape[2]
    heads_here = step_size_bias.shape[1]
    head_size = head_norm_scale.shape[1] // heads_here
    own_rows = local_sequences * fresh_tokens
    active_mask = (jnp.arange(fresh_tokens, dtype=jnp.int32)[None, :] < lengths[:, None]).astype(
        jnp.float32
    )
    group_index = head_rank * heads_here // (STATE_HEADS // G)
    dp_count = lax.axis_size("dp")
    tp_count = lax.axis_size("tp")
    inner = 2 if tp_count % 2 == 0 else 1
    outer = tp_count // inner
    blocks = [partner(seq_rank, k, dp_count) if k else seq_rank for k in range(dp_count)]
    stream = jnp.concatenate(
        [lax.dynamic_slice_in_dim(tokens, blk * own_rows, own_rows, 0) for blk in blocks], axis=0
    ).astype(jnp.float32)
    chip_rank = head_rank // inner
    core_rank = head_rank % inner
    core_pairs = [(r, r ^ 1) for r in range(tp_count)]
    map_cols = maps_weight.shape[3]
    row = jnp.arange(2 * map_cols, dtype=jnp.int32)[:, None]
    col = jnp.arange(2 * N, dtype=jnp.int32)[None, :]
    selectors = []
    for k in range(tp_count):
        step = k % outer
        source_chip = partner(chip_rank, step, outer) if step else chip_rank
        source = source_chip * inner + (core_rank + k // outer) % inner
        hit = (row // map_cols == col // N) & (
            source * map_cols + row % map_cols == G * (col % N) + group_index
        )
        selectors.append(hit.astype(jnp.bfloat16))
    selector = jnp.concatenate(selectors, axis=0)
    input_states, map_states, ssm_states = ([], [], [])
    for layer_number in range(MIXER_LAYERS):
        row_squares = jnp.sum(stream * stream, axis=1)
        squares_high = lax.reduce_precision(row_squares, 8, 7)
        squares_low = row_squares - squares_high
        normed = (stream * input_norm_scale[layer_number]).astype(jnp.bfloat16)
        total_rows = normed.shape[0]
        pair_partial = jnp.einsum(
            "td,dkc->tkc",
            normed,
            gate_input_weight[layer_number],
            preferred_element_type=jnp.float32,
        ).reshape(total_rows, -1)
        maps_partial = jnp.einsum(
            "td,dkc->tkc", normed, maps_weight[layer_number], preferred_element_type=jnp.float32
        ).reshape(total_rows, -1)
        step_partial = jnp.dot(
            normed, step_weight[layer_number], preferred_element_type=jnp.float32
        )
        packed = jnp.concatenate(
            [
                pair_partial.astype(jnp.bfloat16),
                maps_partial.astype(jnp.bfloat16),
                step_partial.astype(jnp.bfloat16),
                squares_high[:, None].astype(jnp.bfloat16),
                squares_low[:, None].astype(jnp.bfloat16),
            ],
            axis=1,
        )
        packed = with_layout_constraint(packed, Layout(major_to_minor=(0, 1)))
        pieces = [packed[k * own_rows : (k + 1) * own_rows] for k in range(dp_count)]
        total = pieces[0].astype(jnp.float32)
        for k in range(1, dp_count):
            total = total + send_to(pieces[k], "dp", k, dp_count).astype(jnp.float32)
        own_factor = lax.rsqrt((total[:, -2:-1] + total[:, -1:]) / D + epsilon)
        wide = pair_partial.shape[1]
        projected = (total[:, :-2] * own_factor).astype(jnp.bfloat16)
        gate_input = projected[:, :wide].reshape(local_sequences, fresh_tokens, 2, wide // 2)
        map_input = projected[:, wide : wide + 2 * map_cols].reshape(
            local_sequences, fresh_tokens, 2, map_cols
        )
        step_raw = projected[:, wide + 2 * map_cols :].reshape(
            local_sequences, fresh_tokens, heads_here
        )
        maps_f, maps_kept = conv_step(
            convolution_map_cache[layer_number], map_input, map_tap_weight[layer_number], lengths
        )
        maps_own = maps_f.astype(jnp.bfloat16).reshape(own_rows, 2 * map_cols)
        maps_all = jnp.concatenate(
            [maps_own] + [take_from(maps_own, "tp", k, outer, inner) for k in range(1, outer)],
            axis=1,
        )
        if inner == 2:
            maps_all = jnp.concatenate(
                [maps_all, lax.ppermute(maps_all, "tp", core_pairs)], axis=1
            )
        conv_input, input_kept = conv_step(
            convolution_input_cache[layer_number],
            gate_input[:, :, 1],
            input_tap_weight[layer_number],
            lengths,
        )
        group_maps = jnp.dot(maps_all, selector, preferred_element_type=jnp.float32).reshape(
            local_sequences, fresh_tokens, 2, N
        )
        write_map = group_maps[:, :, 0]
        read_map = group_maps[:, :, 1]
        head_step_size = (
            jax.nn.softplus(step_raw.astype(jnp.float32) + step_size_bias[layer_number])
            * active_mask[..., None]
        )
        decay_logarithm = (
            head_step_size * -jnp.exp(decay_rate_logarithm[layer_number])
            + extra_log_decay[layer_number] * active_mask[..., None]
        )
        head_input = conv_input.reshape(local_sequences, fresh_tokens, heads_here, head_size)
        head_gate = (
            gate_input[:, :, 0]
            .astype(jnp.float32)
            .reshape(local_sequences, fresh_tokens, heads_here, head_size)
        )
        mixed_out, state_new = ssd_block(
            head_input,
            head_gate,
            head_step_size,
            decay_logarithm,
            write_map,
            read_map,
            recurrent_state[layer_number],
            direct_path_weight[layer_number],
            head_norm_scale[layer_number].reshape(heads_here, head_size),
        )
        ssm_states.append(state_new)
        head_out = (
            (mixed_out * active_mask[:, :, None, None])
            .astype(jnp.bfloat16)
            .reshape(own_rows, heads_here * head_size)
        )
        all_rows = jnp.concatenate(
            [head_out] + [take_from(head_out, "dp", k, dp_count) for k in range(1, dp_count)],
            axis=0,
        )
        partial = jnp.dot(
            all_rows, output_weight[layer_number], preferred_element_type=jnp.float32
        )
        part_rows = total_rows // inner
        part = lax.dynamic_slice_in_dim(partial, core_rank * part_rows, part_rows, 0)
        if inner == 2:
            other = lax.dynamic_slice_in_dim(partial, (1 - core_rank) * part_rows, part_rows, 0)
            swapped = lax.ppermute(other.astype(jnp.bfloat16), "tp", core_pairs)
            part = part + swapped.astype(jnp.float32)
        rounded = part.astype(jnp.bfloat16)
        terms = [rounded] + [take_from(rounded, "tp", k, outer, inner) for k in range(1, outer)]
        terms = [t.astype(jnp.float32) for t in terms]
        while len(terms) > 1:
            terms = [
                terms[i] + terms[i + 1] if i + 1 < len(terms) else terms[i]
                for i in range(0, len(terms), 2)
            ]
        if layer_number == MIXER_LAYERS - 1:
            stacked, terms[0] = lax.optimization_barrier((jnp.stack(ssm_states), terms[0]))
        summed = terms[0].astype(jnp.bfloat16)
        if inner == 2:
            twin = lax.ppermute(summed, "tp", core_pairs)
            first = core_rank == 0
            summed = jnp.concatenate(
                [jnp.where(first, summed, twin), jnp.where(first, twin, summed)], axis=0
            )
        stream = stream + summed.astype(jnp.float32)
        input_states.append(input_kept)
        map_states.append(maps_kept)
    power = dp_count & (dp_count - 1) == 0
    held = [(k ^ seq_rank) if power else (k - seq_rank) % dp_count for k in range(dp_count)]
    ordered = jnp.concatenate(
        [lax.dynamic_slice_in_dim(stream, at * own_rows, own_rows, 0) for at in held], axis=0
    )
    return (ordered, jnp.stack(input_states), jnp.stack(map_states), stacked)


def solution(mesh):
    placed = (
        P(None, "dp"),
        P("dp"),
        P(None, "dp"),
        P(None, "dp", None, "tp"),
        P(None, "dp", None, "tp"),
        P(None, "dp", "tp"),
        P(None, None, "tp"),
        P(None, None, None, "tp"),
        P(None, "tp"),
        P(None, "tp"),
        P(None, "tp"),
        P(None, "tp"),
        P(None, "tp", "dp"),
        P(None, "dp", None, "tp"),
        P(None, "dp", None, None, "tp"),
        P(None, "dp", "tp", None, None),
        P(None, "dp", None, "tp"),
    )
    return jax.shard_map(
        body,
        mesh=mesh,
        in_specs=placed,
        out_specs=(
            P(None, "dp"),
            P(None, "dp", None, "tp"),
            P(None, "dp", None, None, "tp"),
            P(None, "dp", "tp", None, None),
        ),
        check_vma=False,
    )
```
